32 devices in a mesh: sp: 8 (over z, x), tp: 4 (over y, core).
Axes of the slice: x: 2, y: 2, z: 4, core: 2. Of those that a mesh axis runs over, the one named last changes fastest.
Arguments:
- queries: bfloat16 [2048, 1024], P('sp', 'tp'), may hold values from -6 to 6
- keys: bfloat16 [2048, 256], P('sp'), may hold values from -6 to 6
- values: bfloat16 [2048, 256], P('sp'), may hold values from -6 to 6
- sink: float32 [16], P('tp'), may hold values from 3 to 6
- w_out: bfloat16 [1024, 2048], P('tp'), may hold values from -0.1875 to 0.1875
- stream: bfloat16 [2048, 2048], P(('sp', 'tp')), may hold values from -6 to 6
- gain: bfloat16 [2048], replicated, may hold values from 0.099609375 to 1.8984375
- routes: int32 [2048, 4], P('sp'), may hold values from 0 to 63, all different within a row; in each aligned block of 64 rows (0 to 63, 64 to 127, ...) at most 8 rows name the same one
- route_weights: float32 [2048, 4], P('sp'), may hold values from 0.2 to 1
- w_gate: bfloat16 [64, 1024, 2048], P('sp', 'tp'), may hold values from -0.125 to 0.125
- w_up: bfloat16 [64, 1024, 2048], P('sp', 'tp'), may hold values from -0.125 to 0.125
- w_down: bfloat16 [64, 1024, 2048], P('sp', None, 'tp'), may hold values from -0.1875 to 0.1875
- shared_gate: bfloat16 [1024, 2048], P('tp'), may hold values from -0.125 to 0.125
- shared_up: bfloat16 [1024, 2048], P('tp'), may hold values from -0.125 to 0.125
- shared_down: bfloat16 [1024, 2048], P(None, 'tp'), may hold values from -0.1875 to 0.1875
Outputs:
- layer_out: bfloat16 [2048, 2048], P('sp', 'tp')
The draws below stay inside these ranges and needn't reach their ends.
Inputs may be any that keep to these rules, and one draw needn't show every extreme that they name: `routes`: in each aligned block of 64 rows no expert is named in more than 8 rows, and some blocks reach 8; a row names 4 different experts.
All inputs are finite; a program needn't handle non-finite values.
Results may differ from the reference program's by a relative error of at most 0.014.
Values may be sent and summed in bfloat16 or wider, within the bound.
No kernel may reach another device: no remote copies, remote signals or barrier semaphores. Data moves between devices by JAX's collectives and lax.ppermute only.
A program may use at most 128 MiB of HBM per device.

```python
import math
import jax
import jax.numpy as jnp
import numpy as np
from jax import lax

D = 2048
HEADS = 16
KV_HEADS = 4
HD = 64
WINDOW = 128
EXPERTS = 64
TOPK = 4
FE = 1024
FS = 1024
TOKENS = 2048
ROWS_DEV = 64
CAP = 8
N_SP = 8
N_TP = 4


def draw_queries(key, part):
    base_key = jax.random.fold_in(key, 1)
    base_draw = jax.random.truncated_normal(base_key, -6.0, 6.0, (TOKENS, HEADS, HD), jnp.float32)
    return base_draw.reshape(TOKENS, HEADS * HD).astype(jnp.bfloat16)


def draw_keys(key, part):
    base_key = jax.random.fold_in(key, 2)
    base_draw = jax.random.truncated_normal(base_key, -6.0, 6.0, (TOKENS, KV_HEADS, HD), jnp.float32)
    return base_draw.reshape(TOKENS, KV_HEADS * HD).astype(jnp.bfloat16)


def block_levels(stream_key, extent, pieces, smallest, high):
    def one(dim, blocks):
        heights = jax.random.uniform(jax.random.fold_in(jax.random.fold_in(stream_key, 6), dim), (blocks,), jnp.float32, smallest / len(pieces), high / len(pieces))
        return jnp.repeat(jnp.exp(heights), extent[dim] // blocks).reshape((-1,) + (1,) * (len(extent) - dim - 1))

    factor_of = one(*pieces[0])
    for cut in pieces[1:]:
        factor_of = factor_of * one(*cut)
    return factor_of


def deal_out(stream_key, own, number, rows, amount, top, reach, lean):
    order = jax.random.permutation(stream_key, amount)
    packed, usual = portions_of(amount, rows * top, reach, lean, True), portions_of(amount, rows * top, reach, lean, False)
    places = jnp.arange(amount)

    def named(sizes, rotation):
        used = int((sizes > 0).sum())
        fixed = max(1, used // 4)
        passed = fixed + (places - fixed + rotation * (used - fixed)) % max(1, amount - fixed)
        return jnp.zeros((amount,), jnp.int32).at[order[jnp.where(places < fixed, places, passed)]].set(jnp.asarray(sizes, jnp.int32))

    sizes = jnp.where(number % 4 == 0, named(packed, number // 4), named(usual, number - number // 4 - 1))
    mixed = jax.random.permutation(jax.random.fold_in(own, 3), amount)
    giver, taker = mixed[0:amount // 2 * 2:2], mixed[1:amount // 2 * 2:2]
    room = jnp.minimum(sizes[giver] - 1, reach - sizes[taker]) // 2
    room = jnp.where((giver == order[0]) | (taker == order[0]) | (sizes[taker] == 0), 0, jnp.maximum(room, 0))
    passed = jax.random.randint(jax.random.fold_in(own, 4), (amount // 2,), 0, 1 << 20) % (room + 1)
    sizes = sizes.at[giver].add(-passed).at[taker].add(passed)
    items = jnp.searchsorted(jnp.cumsum(sizes), jnp.arange(rows * top), side="right").astype(jnp.int32)
    grid = items.reshape(top, rows).T
    grid = grid[jax.random.permutation(jax.random.fold_in(own, 1), rows)]
    rotation = jax.random.randint(jax.random.fold_in(own, 2), (rows, 1), 0, top)
    return jnp.take_along_axis(grid, (jnp.arange(top)[None, :] + rotation) % top, axis=1)


def portions_of(amount, total, bound, skew, full):
    portions = [(1 << 20) // math.isqrt(grade ** skew) + 1 for grade in range(1, amount + 1)]
    largest = bound if full else min(bound, max(-(-total // amount), total * portions[0] // sum(portions)))
    least = 1 if total - largest >= amount - 1 else 0
    given, surplus = [largest] + [least] * (amount - 1), total - largest - least * (amount - 1)
    while surplus > 0:
        candidates = [i for i in range(1, amount) if given[i] < largest] or [i for i in range(1, amount) if given[i] < bound]
        mass, left = sum([portions[i] for i in candidates]), surplus
        for i in candidates:
            addition = min(bound - given[i], max(1, left * portions[i] // mass), surplus)
            given[i] = given[i] + addition
            surplus = surplus - addition
    return np.array(given)


def bell_draw(rng, dims, scale, reach, cuts=(), dtype=jnp.bfloat16):
    level = block_levels(rng, dims, cuts, -0.22, 0.18) if cuts else 1.0
    result = jax.random.normal(rng, dims, jnp.float32) * scale * level
    return jnp.minimum(jnp.maximum(result, -reach), reach).astype(dtype)


def setup_inputs(seed: int = 0) -> dict:
    arg_keys = jax.random.split(jax.random.key(seed), 16)
    queries = draw_queries(jax.random.fold_in(arg_keys[15], 71), 0)
    keys = draw_keys(jax.random.fold_in(arg_keys[15], 71), 0)
    values = bell_draw(arg_keys[2], (TOKENS, KV_HEADS * HD), 1.0, 6.0, ((0, 8),))
    sink = jnp.clip(3.0 + 3.0 * jax.random.uniform(arg_keys[3], (HEADS,), jnp.float32) ** block_levels(arg_keys[3], (HEADS,), ((0, 4),), -0.2, 0.2), 3.0, 6.0)
    w_out = bell_draw(arg_keys[4], (HEADS * HD, D), (HEADS * HD) ** -0.5, 0.1875, ((0, 4),))
    stream = bell_draw(arg_keys[5], (TOKENS, D), 1.0, 6.0, ((0, 32),))
    gain = jnp.clip(1.0 + 0.18 * jax.random.normal(arg_keys[6], (D,), jnp.float32), 0.099609375, 1.8984375).astype(jnp.bfloat16)
    routes_keys = jax.random.split(jax.random.fold_in(arg_keys[7], 1), TOKENS // ROWS_DEV)
    routes_turns = jax.random.permutation(jax.random.fold_in(arg_keys[7], 3), TOKENS // ROWS_DEV)
    routes = jax.vmap(lambda own, number: deal_out(jax.random.fold_in(arg_keys[7], 2), own, number, ROWS_DEV, EXPERTS, TOPK, CAP, 2))(routes_keys, routes_turns).reshape((TOKENS, TOPK))
    route_weights = jnp.clip(0.2 + 0.8 * jax.random.uniform(arg_keys[8], (TOKENS, TOPK), jnp.float32) ** block_levels(arg_keys[8], (TOKENS, TOPK), ((0, 8),), -0.2, 0.2), 0.2, 1.0)
    w_gate = bell_draw(arg_keys[9], (EXPERTS, FE, D), D ** -0.5, 0.125, ((0, 8), (1, 4)))
    w_up = bell_draw(arg_keys[10], (EXPERTS, FE, D), D ** -0.5, 0.125, ((0, 8), (1, 4)))
    w_down = bell_draw(arg_keys[11], (EXPERTS, FE, D), FE ** -0.5, 0.1875, ((0, 8), (2, 4)))
    shared_gate = bell_draw(arg_keys[12], (FS, D), D ** -0.5, 0.125, ((0, 4),))
    shared_up = bell_draw(arg_keys[13], (FS, D), D ** -0.5, 0.125, ((0, 4),))
    shared_down = bell_draw(arg_keys[14], (FS, D), FS ** -0.5, 0.1875, ((1, 4),))
    return dict(queries=queries, keys=keys, values=values, sink=sink, w_out=w_out, stream=stream, gain=gain, routes=routes, route_weights=route_weights, w_gate=w_gate, w_up=w_up, w_down=w_down, shared_gate=shared_gate, shared_up=shared_up, shared_down=shared_down)


NORM_EPS = 1e-05

def attention_part(queries, keys, values, sink):
    group = HEADS // KV_HEADS
    blocks = TOKENS // WINDOW
    query_heads = queries.astype(jnp.float32).reshape(blocks, WINDOW, KV_HEADS, group, HD)

    def banded(source):
        padded = jnp.pad(source.astype(jnp.float32).reshape(TOKENS, KV_HEADS, HD), ((WINDOW, WINDOW), (0, 0), (0, 0)))
        framed = padded.reshape(blocks + 2, WINDOW, KV_HEADS, HD)
        return jnp.concatenate([framed[:-2], framed[1:-1], framed[2:]], axis=1)
    key_band = banded(keys)
    value_band = banded(values)
    scores = jnp.einsum('nqkgd,njkd->nkgqj', query_heads, key_band, precision=lax.Precision.HIGHEST) * HD ** (-0.5)
    query_pos = jnp.arange(blocks)[:, None, None] * WINDOW + jnp.arange(WINDOW)[None, :, None]
    key_pos = jnp.arange(blocks)[:, None, None] * WINDOW - WINDOW + jnp.arange(3 * WINDOW)[None, None, :]
    allowed = (jnp.abs(query_pos - key_pos) <= WINDOW) & (key_pos >= 0) & (key_pos < TOKENS)
    scores = jnp.where(allowed[:, None, None], scores, -jnp.inf)
    sink_level = sink.astype(jnp.float32).reshape(1, KV_HEADS, group, 1, 1)
    row_peak = jnp.maximum(scores.max(-1, keepdims=True), sink_level)
    probabilities = jnp.exp(scores - row_peak)
    denominator = probabilities.sum(-1, keepdims=True) + jnp.exp(sink_level - row_peak)
    rounded = lax.optimization_barrier((probabilities / denominator).astype(jnp.bfloat16)).astype(jnp.float32)
    attended = jnp.einsum('nkgqj,njkd->nqkgd', rounded, value_band, precision=lax.Precision.HIGHEST)
    return attended.astype(jnp.bfloat16).reshape(TOKENS, HEADS * HD)

def routed_part(normed, routes, route_weights, w_gate, w_up, w_down):
    most_rows = N_SP * N_TP * CAP
    flat_routes = routes.reshape(-1).astype(jnp.int32)
    flat_weights = route_weights.reshape(-1).astype(jnp.float32)
    sorted_ids = jnp.argsort(flat_routes, stable=True).astype(jnp.int32)
    counts = lax.optimization_barrier(jnp.sum((flat_routes[:, None] == jnp.arange(EXPERTS)[None, :]).astype(jnp.int32), axis=0))
    starts = (jnp.cumsum(counts) - counts).astype(jnp.int32)
    padded = jnp.concatenate([sorted_ids, jnp.zeros((most_rows,), jnp.int32)])

    def one_expert(accumulated, expert):
        picked = lax.dynamic_slice(padded, (starts[expert].astype(jnp.int32),), (most_rows,))
        is_valid = jnp.arange(most_rows) < counts[expert]
        token_ids = (picked // TOPK).astype(jnp.int32)
        picked_rows = normed[token_ids]
        gate_act = jnp.dot(picked_rows, w_gate[expert].T, preferred_element_type=jnp.float32)
        up_act = jnp.dot(picked_rows, w_up[expert].T, preferred_element_type=jnp.float32)
        hidden = (jax.nn.silu(gate_act) * up_act).astype(jnp.bfloat16)
        expert_out = jnp.dot(hidden, w_down[expert], preferred_element_type=jnp.float32)
        expert_out = lax.optimization_barrier(expert_out.astype(jnp.bfloat16)).astype(jnp.float32)
        scale_col = jnp.where(is_valid, flat_weights[picked], 0.0).astype(jnp.float32)
        return (accumulated.at[token_ids].add(expert_out * scale_col[:, None]), None)
    total_init = jnp.zeros((TOKENS, D), jnp.float32)
    routed, unused = lax.scan(one_expert, total_init, jnp.arange(EXPERTS))
    return routed

def reference(queries, keys, values, sink, w_out, stream, gain, routes, route_weights, w_gate, w_up, w_down, shared_gate, shared_up, shared_down):
    attended = attention_part(queries, keys, values, sink)
    projected = jnp.dot(attended, w_out, preferred_element_type=jnp.float32)
    mixed_rows = (stream.astype(jnp.float32) + projected).astype(jnp.bfloat16)
    wide_rows = mixed_rows.astype(jnp.float32)
    scale_rows = lax.rsqrt(lax.optimization_barrier(jnp.mean(wide_rows * wide_rows, axis=-1, keepdims=True)) + NORM_EPS)
    normed = (wide_rows * scale_rows * gain.astype(jnp.float32)).astype(jnp.bfloat16)
    routed = routed_part(normed, routes, route_weights, w_gate, w_up, w_down)
    shared_gate_act = jnp.dot(normed, shared_gate.T, preferred_element_type=jnp.float32)
    shared_up_act = jnp.dot(normed, shared_up.T, preferred_element_type=jnp.float32)
    shared_hidden = (jax.nn.silu(shared_gate_act) * shared_up_act).astype(jnp.bfloat16)
    shared_out = jnp.dot(shared_hidden, shared_down, preferred_element_type=jnp.float32)
    return (wide_rows + routed + shared_out).astype(jnp.bfloat16)
```

```python
import functools

import jax
import jax.numpy as jnp
from jax import lax
from jax.experimental import pallas as pl
from jax.experimental.pallas import tpu as pltpu
from jax.sharding import PartitionSpec as P

D = 2048
HEADS = 16
KV_HEADS = 4
HD = 64
WINDOW = 128
EXPERTS = 64
TOPK = 4


NORM_EPS = 1e-05
LANES = 128


def with_halo(array, sides, width):
    for axis, dim in sides:
        devices, length = (lax.axis_size(axis), array.shape[dim])
        up = [(i, (i + 1) % devices) for i in range(devices - 1)]
        down = [(j, i) for i, j in up]
        last = lax.slice_in_dim(array, length - width, length, axis=dim)
        leading = lax.slice_in_dim(array, 0, width, axis=dim)
        before = lax.ppermute(last, axis, up)
        after = lax.ppermute(leading, axis, down)
        array = jnp.concatenate([before, array, after], axis=dim)
    return array


def slot_ids(block_routes, capacity):
    flat_routes = block_routes.reshape(-1)
    hit_table = (flat_routes[:, None] == jnp.arange(EXPERTS)[None, :]).astype(jnp.int32)
    earlier = jnp.cumsum(hit_table, axis=0) - hit_table
    slot_rank = jnp.sum(earlier * hit_table, axis=1)
    return flat_routes * capacity + slot_rank


def attention(queries, keys, values, sink):
    tok_dev = queries.shape[0]
    n_tp = lax.axis_size("tp")
    n_sp = lax.axis_size("sp")
    tp_idx = lax.axis_index("tp")
    sp_idx = lax.axis_index("sp")
    heads_dev = HEADS // n_tp
    group = HEADS // KV_HEADS
    kv_head = tp_idx * heads_dev // group
    key_own = lax.dynamic_slice_in_dim(keys, kv_head * HD, HD, 1)
    value_own = lax.dynamic_slice_in_dim(values, kv_head * HD, HD, 1)
    paired = jnp.concatenate([key_own, value_own], axis=1)
    padded = with_halo(paired, (("sp", 0),), WINDOW)
    blocks = tok_dev // WINDOW
    framed = padded.reshape(blocks + 2, WINDOW, 2 * HD)
    banded = jnp.concatenate([framed[:-2], framed[1:-1], framed[2:]], axis=1)
    key_band = banded[:, :, :HD]
    value_band = banded[:, :, HD:]
    query_blocks = queries.reshape(blocks, WINDOW, heads_dev, HD)
    scores = jnp.einsum(
        "nqhd,njd->nhqj", query_blocks, key_band, preferred_element_type=jnp.float32
    ) * HD ** (-0.5)
    offset = sp_idx * tok_dev
    seq_total = tok_dev * n_sp
    query_pos = (
        offset + jnp.arange(blocks)[:, None, None] * WINDOW + jnp.arange(WINDOW)[None, :, None]
    )
    key_pos = (
        offset
        - WINDOW
        + jnp.arange(blocks)[:, None, None] * WINDOW
        + jnp.arange(3 * WINDOW)[None, None, :]
    )
    allowed = (jnp.abs(query_pos - key_pos) <= WINDOW) & (key_pos >= 0) & (key_pos < seq_total)
    scores = jnp.where(allowed[:, None], scores, -jnp.inf)
    sink_level = sink.reshape(1, heads_dev, 1, 1)
    row_peak = jnp.maximum(scores.max(-1, keepdims=True), sink_level)
    probabilities = jnp.exp(scores - row_peak)
    denominator = probabilities.sum(-1, keepdims=True) + jnp.exp(sink_level - row_peak)
    weights = (probabilities / denominator).astype(jnp.bfloat16)
    attended = jnp.einsum("nhqj,njd->nqhd", weights, value_band, preferred_element_type=jnp.float32)
    return attended.astype(jnp.bfloat16).reshape(tok_dev, heads_dev * HD)


def local_general(
    queries,
    keys,
    values,
    sink,
    w_out,
    stream,
    gain,
    routes,
    route_weights,
    w_gate,
    w_up,
    w_down,
    shared_gate,
    shared_up,
    shared_down,
):
    tok_dev = queries.shape[0]
    n_tp = lax.axis_size("tp")
    n_sp = lax.axis_size("sp")
    tp_idx = lax.axis_index("tp")
    attended = attention(queries, keys, values, sink)
    rows_dev = tok_dev // n_tp
    d_dev = w_down.shape[2]
    projected = lax.psum_scatter(
        jnp.dot(attended, w_out, preferred_element_type=jnp.float32),
        "tp",
        scatter_dimension=0,
        tiled=True,
    )
    mixed_rows = (stream.astype(jnp.float32) + projected).astype(jnp.bfloat16)
    whole_rows = lax.all_gather(mixed_rows, "tp", axis=0, tiled=True)
    wide_rows = whole_rows.astype(jnp.float32)
    scale_rows = lax.rsqrt(jnp.mean(wide_rows * wide_rows, axis=-1, keepdims=True) + NORM_EPS)
    normed = (wide_rows * scale_rows * gain.astype(jnp.float32)).astype(jnp.bfloat16)
    residual = lax.dynamic_slice_in_dim(wide_rows, tp_idx * d_dev, d_dev, 1)
    exp_dev = w_gate.shape[0]
    capacity = max(1, 2 * tok_dev * TOPK // (n_tp * EXPERTS))
    slot_count = EXPERTS * capacity
    blocked_routes = routes.reshape(n_tp, rows_dev, TOPK)
    destination = jax.vmap(lambda block_routes: slot_ids(block_routes, capacity))(blocked_routes)
    slot_select = destination[:, None, :] == jnp.arange(slot_count)[None, :, None]
    slot_select = slot_select.reshape(n_tp, slot_count, rows_dev, TOPK).astype(jnp.float32)
    dispatch_table = jnp.sum(slot_select, axis=-1).astype(jnp.bfloat16)
    combine_table = jnp.sum(slot_select * route_weights.reshape(n_tp, 1, rows_dev, TOPK), axis=-1)
    normed_blocks = normed.reshape(n_tp, rows_dev, D)
    own_table = lax.dynamic_index_in_dim(dispatch_table, tp_idx, 0, keepdims=False)
    own_rows = lax.dynamic_index_in_dim(normed_blocks, tp_idx, 0, keepdims=False)
    outgoing = jnp.dot(own_table, own_rows, preferred_element_type=jnp.float32).astype(jnp.bfloat16)
    arrived = lax.all_to_all(outgoing, "sp", split_axis=0, concat_axis=0, tiled=True)
    arrived = arrived.reshape(1, n_sp, exp_dev, capacity, D)
    piece_rows = lax.all_gather(arrived, "tp", axis=0, tiled=True)
    gate_act = jnp.einsum(
        "tsecd,efd->tsecf", piece_rows, w_gate, preferred_element_type=jnp.float32
    )
    up_act = jnp.einsum("tsecd,efd->tsecf", piece_rows, w_up, preferred_element_type=jnp.float32)
    hidden = (jax.nn.silu(gate_act) * up_act).astype(jnp.bfloat16)
    shared_gate_act = jnp.einsum(
        "td,fd->tf", normed, shared_gate, preferred_element_type=jnp.float32
    )
    shared_up_act = jnp.einsum("td,fd->tf", normed, shared_up, preferred_element_type=jnp.float32)
    shared_hidden = (jax.nn.silu(shared_gate_act) * shared_up_act).astype(jnp.bfloat16)
    shared_hidden = shared_hidden.reshape(1, 1, 1, tok_dev, shared_hidden.shape[1])
    expert_piece = lax.all_gather(hidden, "tp", axis=4, tiled=True)
    shared_piece = lax.all_gather(shared_hidden, "tp", axis=4, tiled=True)
    piece_width = expert_piece.shape[4]
    routed_total = jnp.einsum(
        "tsecf,efd->tsecd", expert_piece, w_down, preferred_element_type=jnp.float32
    )
    shared_total = jnp.dot(
        shared_piece.reshape(tok_dev, piece_width), shared_down, preferred_element_type=jnp.float32
    )
    returned = lax.all_to_all(
        routed_total.astype(jnp.bfloat16), "sp", split_axis=1, concat_axis=1, tiled=True
    )
    returned = returned.reshape(n_tp, slot_count, d_dev).astype(jnp.float32)
    routed = jnp.einsum("tmr,tmd->trd", combine_table, returned, precision=lax.Precision.HIGHEST)
    routed = routed.reshape(tok_dev, d_dev)
    return (residual + routed + shared_total).astype(jnp.bfloat16)


NT = (((1,), (1,)), ((), ()))
TN = (((0,), (0,)), ((), ()))


def silu_product(gate, up):
    return (gate / (1.0 + jnp.exp(-gate)) * up).astype(jnp.bfloat16)


def up_kernel(where_ref, *refs, units, quads, exp_dev, capacity, rows):
    count = units * quads
    pieces = refs[:count]
    gate_ref, up_ref, sgate_ref, sup_ref, hidden_ref, high_ref, low_ref, slots_ref = refs[count:]
    step = pl.program_id(0)
    width = quads * capacity
    lanes = exp_dev * width

    @pl.when(step == 0)
    def _():
        first = where_ref[0].astype(jnp.float32)
        lane = lax.broadcasted_iota(jnp.int32, (rows, lanes), 1).astype(jnp.float32)
        for unit in range(units):
            tables, tokens = [], []
            for quad in range(quads):
                piece = pieces[unit * quads + quad]
                spot = where_ref[1] ^ quad
                extra = piece[:, D:].astype(jnp.float32)
                place = (
                    (extra[:, 0:TOPK] - first) * width
                    + spot.astype(jnp.float32) * capacity
                    + extra[:, TOPK : 2 * TOPK]
                )
                table = jnp.zeros((rows, lanes), jnp.float32)
                high = jnp.zeros((rows, lanes), jnp.float32)
                low = jnp.zeros((rows, lanes), jnp.float32)
                for k in range(TOPK):
                    hit = place[:, k : k + 1] == lane
                    table = jnp.where(hit, 1.0, table)
                    high = jnp.where(hit, extra[:, 2 * TOPK + k : 2 * TOPK + k + 1], high)
                    low = jnp.where(hit, extra[:, 3 * TOPK + k : 3 * TOPK + k + 1], low)
                start = pl.multiple_of(spot * rows, rows)
                high_ref[unit, pl.ds(start, rows), :] = high.astype(jnp.bfloat16)
                low_ref[unit, pl.ds(start, rows), :] = low.astype(jnp.bfloat16)
                tables.append(table.astype(jnp.bfloat16))
                tokens.append(piece[:, :D])
            picked = lax.dot_general(
                jnp.concatenate(tables, axis=0),
                jnp.concatenate(tokens, axis=0),
                TN,
                preferred_element_type=jnp.float32,
            ).astype(jnp.bfloat16)
            for e in range(exp_dev):
                slots_ref[e, unit * width : (unit + 1) * width, :] = picked[
                    e * width : (e + 1) * width
                ]
        for quad in range(quads):
            own = pieces[quad][:, :D]
            gate = lax.dot_general(own, sgate_ref[...], NT, preferred_element_type=jnp.float32)
            up = lax.dot_general(own, sup_ref[...], NT, preferred_element_type=jnp.float32)
            start = pl.multiple_of((where_ref[1] ^ quad) * rows, rows)
            hidden_ref[0, pl.ds(start, rows), :] = silu_product(gate, up)

    @pl.when(step > 0)
    def _():
        held = slots_ref[step - 1]
        gate = lax.dot_general(held, gate_ref[0], NT, preferred_element_type=jnp.float32)
        up = lax.dot_general(held, up_ref[0], NT, preferred_element_type=jnp.float32)
        hidden_ref[0] = silu_product(gate, up)


def down_kernel(where_ref, *refs, units, quads, exp_dev, capacity, rows, piece):
    hiddens = refs[:quads]
    down_ref, sdown_ref, high_ref, low_ref, shared_ref = refs[quads : quads + 5]
    outs = refs[quads + 5 : quads + 5 + units]
    result_ref = refs[-1]
    step = pl.program_id(0)
    width = quads * capacity

    def product(weight_ref, lead):
        total = None
        for quad in range(quads):
            start = pl.multiple_of((where_ref[1] ^ quad) * piece, piece)
            weight = weight_ref[lead + (pl.ds(start, piece), slice(None))]
            part = jnp.dot(hiddens[quad][0], weight, preferred_element_type=jnp.float32)
            total = part if total is None else total + part
        return total

    @pl.when(step == 0)
    def _():
        shared_ref[...] = product(sdown_ref, ())

    @pl.when(step > 0)
    def _():
        total = product(down_ref, (0,)).astype(jnp.bfloat16)
        start = pl.multiple_of((step - 1) * width, width)
        for unit in range(units):
            result_ref[unit, pl.ds(start, width), :] = total[unit * width : (unit + 1) * width]

    @pl.when(step == exp_dev)
    def _():
        for unit in range(units):
            held = result_ref[unit]
            routed = jnp.dot(high_ref[unit], held, preferred_element_type=jnp.float32)
            routed += jnp.dot(low_ref[unit], held, preferred_element_type=jnp.float32)
            outs[unit][...] = routed.astype(jnp.bfloat16)


def whole(shape):
    return pl.BlockSpec(shape, lambda i, w: (0,) * len(shape), pipeline_mode=pl.Buffered(1))


def local_torus(
    queries,
    keys,
    values,
    sink,
    w_out,
    stream,
    gain,
    routes,
    route_weights,
    w_gate,
    w_up,
    w_down,
    shared_gate,
    shared_up,
    shared_down,
    *,
    nx,
):
    tok_dev = queries.shape[0]
    n_tp = lax.axis_size("tp")
    n_sp = lax.axis_size("sp")
    nz = n_sp // nx
    tp_idx = lax.axis_index("tp")
    sp_idx = lax.axis_index("sp")
    rows = tok_dev // n_tp
    d_dev = w_down.shape[2]
    exp_dev = w_gate.shape[0]
    piece = w_gate.shape[1]
    capacity = max(1, 2 * tok_dev * TOPK // (n_tp * EXPERTS))
    bf16, f32 = jnp.bfloat16, jnp.float32

    def core_swap(a):
        return lax.ppermute(a, "tp", [(i, i ^ 1) for i in range(n_tp)])

    def y_swap(a):
        return lax.ppermute(a, "tp", [(i, i ^ 2) for i in range(n_tp)])

    def x_swap(a):
        return lax.ppermute(a, "sp", [(i, i ^ 1) for i in range(n_sp)])

    def z_from(a, k):
        return lax.ppermute(a, "sp", [((i + k * nx) % n_sp, i) for i in range(n_sp)])

    def z_to(a, k):
        return lax.ppermute(a, "sp", [(i, (i + k * nx) % n_sp) for i in range(n_sp)])

    own_routes = lax.dynamic_slice_in_dim(routes, tp_idx * rows, rows, 0)
    own_weights = lax.dynamic_slice_in_dim(route_weights, tp_idx * rows, rows, 0)
    hits = own_routes[:, :, None] == jnp.arange(EXPERTS)[None, None, :]
    named = jnp.any(hits, axis=1).astype(bf16)
    earlier = (jnp.arange(rows)[:, None] > jnp.arange(rows)[None, :]).astype(bf16)
    ranks = jnp.dot(earlier, named, preferred_element_type=f32)
    rank = jnp.sum(jnp.where(hits, ranks[:, None, :], 0.0), axis=2)
    weight_high = lax.reduce_precision(own_weights, 8, 7)
    weight_low = lax.reduce_precision(own_weights - weight_high, 8, 7)
    extra = jnp.concatenate([own_routes.astype(f32), rank, weight_high, weight_low], axis=1)
    extra = jnp.pad(extra, ((0, 0), (0, LANES - extra.shape[1]))).astype(bf16)

    attended = attention(queries, keys, values, sink)
    projected = jnp.dot(attended, w_out, preferred_element_type=f32)
    quarters = projected.reshape(n_tp // 2, 2, rows, D)
    core = tp_idx % 2
    own_y = tp_idx // 2
    keep = lax.dynamic_index_in_dim(quarters, core, 1, keepdims=False)
    give = lax.dynamic_index_in_dim(quarters, 1 - core, 1, keepdims=False)
    chip = keep + core_swap(give)
    away = lax.dynamic_index_in_dim(chip, 1 - own_y, 0, keepdims=False).astype(bf16)
    home = lax.dynamic_index_in_dim(chip, own_y, 0, keepdims=False)
    summed = home + y_swap(away).astype(f32)
    mixed = (stream.astype(f32) + summed).astype(bf16)
    wide = mixed.astype(f32)
    scale = lax.rsqrt(jnp.mean(wide * wide, axis=-1, keepdims=True) + NORM_EPS)
    normed = (wide * scale * gain.astype(f32)).astype(bf16)
    own = jnp.concatenate([normed, extra], axis=1)

    z_units = [own] + [z_from(own, k) for k in range(1, nz)]
    pieces = []
    for k, near in enumerate(z_units):
        by_x = x_swap(near)
        by_y = y_swap(near)
        both = x_swap(by_y) if k % 2 == 0 else y_swap(by_x)
        pieces += [[near, by_y], [by_x, both]]
    units = nz * nx
    operands = []
    for first, second in pieces:
        operands += [first, core_swap(first), second, core_swap(second)]
    quads = n_tp

    columns = mixed.reshape(rows, n_tp // 2, 2, d_dev)
    away = lax.dynamic_index_in_dim(columns, 1 - own_y, 1, keepdims=False)
    home = lax.dynamic_index_in_dim(columns, own_y, 1, keepdims=False)
    chip_columns = jnp.stack([home, y_swap(away)], axis=0)
    give = lax.dynamic_index_in_dim(chip_columns, 1 - core, 2, keepdims=False)
    keep = lax.dynamic_index_in_dim(chip_columns, core, 2, keepdims=False)
    both = jnp.stack([keep, core_swap(give)], axis=1)
    both = both.reshape(n_tp, rows, d_dev)
    residual = jnp.take(both, jnp.arange(n_tp) ^ tp_idx, axis=0).reshape(tok_dev, d_dev)

    where = jnp.stack([sp_idx * exp_dev, tp_idx]).astype(jnp.int32)
    slots = units * quads * capacity
    lanes = exp_dev * quads * capacity

    def expert(i, w):
        return (jnp.maximum(i - 1, 0), 0, 0)

    sizes = dict(units=units, quads=quads, exp_dev=exp_dev, capacity=capacity, rows=rows)
    hidden, high, low = pl.pallas_call(
        functools.partial(up_kernel, **sizes),
        grid_spec=pltpu.PrefetchScalarGridSpec(
            num_scalar_prefetch=1,
            grid=(exp_dev + 1,),
            in_specs=[whole((rows, D + LANES))] * (units * quads)
            + [pl.BlockSpec((1, piece, D), expert)] * 2
            + [whole((piece, D))] * 2,
            out_specs=[
                pl.BlockSpec((1, slots, piece), lambda i, w: (i, 0, 0)),
                whole((units, tok_dev, lanes)),
                whole((units, tok_dev, lanes)),
            ],
            scratch_shapes=[pltpu.VMEM((exp_dev, slots, D), bf16)],
        ),
        out_shape=[
            jax.ShapeDtypeStruct((exp_dev + 1, slots, piece), bf16),
            jax.ShapeDtypeStruct((units, tok_dev, lanes), bf16),
            jax.ShapeDtypeStruct((units, tok_dev, lanes), bf16),
        ],
        compiler_params=pltpu.CompilerParams(vmem_limit_bytes=56 * 1024 * 1024),
        name="up_kernel",
    )(where, *operands, w_gate, w_up, shared_gate, shared_up)

    hidden_core = core_swap(hidden)
    hidden_y = y_swap(hidden)
    hidden_both = core_swap(hidden_y)

    down = pl.pallas_call(
        functools.partial(down_kernel, piece=piece, **sizes),
        grid_spec=pltpu.PrefetchScalarGridSpec(
            num_scalar_prefetch=1,
            grid=(exp_dev + 1,),
            in_specs=[pl.BlockSpec((1, slots, piece), lambda i, w: (i, 0, 0))] * quads
            + [
                pl.BlockSpec((1, quads * piece, d_dev), expert),
                whole((quads * piece, d_dev)),
                whole((units, tok_dev, lanes)),
                whole((units, tok_dev, lanes)),
            ],
            out_specs=[whole((tok_dev, d_dev))] * (1 + units),
            scratch_shapes=[pltpu.VMEM((units, lanes, d_dev), bf16)],
        ),
        out_shape=[jax.ShapeDtypeStruct((tok_dev, d_dev), f32)]
        + [jax.ShapeDtypeStruct((tok_dev, d_dev), bf16)] * units,
        compiler_params=pltpu.CompilerParams(vmem_limit_bytes=48 * 1024 * 1024),
        name="down_kernel",
    )(where, hidden, hidden_core, hidden_y, hidden_both, w_down, shared_down, high, low)
    shared_total, parts = down[0], down[1:]

    total = residual.astype(f32) + shared_total
    for k in range(nz):
        sum_x = parts[k * nx].astype(f32) + x_swap(parts[k * nx + 1]).astype(f32)
        total += sum_x if k == 0 else z_to(sum_x.astype(bf16), k).astype(f32)
    return total.astype(bf16)


def solution(mesh):
    placed = (
        P("sp", "tp"),
        P("sp", None),
        P("sp", None),
        P("tp"),
        P("tp", None),
        P(("sp", "tp"), None),
        P(),
        P("sp", None),
        P("sp", None),
        P("sp", "tp", None),
        P("sp", "tp", None),
        P("sp", None, "tp"),
        P("tp", None),
        P("tp", None),
        P(None, "tp"),
    )
    n_sp, n_tp = mesh.shape["sp"], mesh.shape["tp"]
    nx = 1
    while 4 * nx * nx <= n_sp:
        nx *= 2

    def local(*args):
        tok_dev, piece = args[0].shape[0], args[9].shape[1]
        capacity = 2 * tok_dev * TOPK // (n_tp * EXPERTS)
        pairs = nx == 2 and n_tp == 4 and n_sp % nx == 0 and n_sp >= 4
        tiles = capacity % 8 == 0 and piece % LANES == 0 and (tok_dev // n_tp) % 16 == 0
        slots = n_sp * n_tp * capacity == tok_dev
        if pairs and tiles and slots:
            return local_torus(*args, nx=nx)
        return local_general(*args)

    return jax.shard_map(
        local, mesh=mesh, in_specs=placed, out_specs=P("sp", "tp"), check_vma=False
    )
```

```python
import functools

import jax
import jax.numpy as jnp
from jax import lax
from jax.experimental import pallas as pl
from jax.experimental.pallas import tpu as pltpu
from jax.sharding import PartitionSpec as P


D = 2048
HEADS = 16
KV_HEADS = 4
HD = 64
WINDOW = 128
EXPERTS = 64
TOPK = 4


NORM_EPS = 1e-05
LANES = 128
AHEAD = 2
DOWN_AHEAD = 4
UP_VMEM = 36 * 1024 * 1024
DOWN_VMEM = 20 * 1024 * 1024


def with_halo(array, sides, width):
    for axis, dim in sides:
        devices, length = (lax.axis_size(axis), array.shape[dim])
        up = [(i, (i + 1) % devices) for i in range(devices - 1)]
        down = [(j, i) for i, j in up]
        last = lax.slice_in_dim(array, length - width, length, axis=dim)
        leading = lax.slice_in_dim(array, 0, width, axis=dim)
        before = lax.ppermute(last, axis, up)
        after = lax.ppermute(leading, axis, down)
        array = jnp.concatenate([before, array, after], axis=dim)
    return array


def slot_ids(block_routes, capacity):
    flat_routes = block_routes.reshape(-1)
    hit_table = (flat_routes[:, None] == jnp.arange(EXPERTS)[None, :]).astype(jnp.int32)
    earlier = jnp.cumsum(hit_table, axis=0) - hit_table
    slot_rank = jnp.sum(earlier * hit_table, axis=1)
    return flat_routes * capacity + slot_rank


def attention(queries, keys, values, sink):
    tok_dev = queries.shape[0]
    n_tp = lax.axis_size("tp")
    n_sp = lax.axis_size("sp")
    tp_idx = lax.axis_index("tp")
    sp_idx = lax.axis_index("sp")
    heads_dev = HEADS // n_tp
    group = HEADS // KV_HEADS
    kv_head = tp_idx * heads_dev // group
    key_own = lax.dynamic_slice_in_dim(keys, kv_head * HD, HD, 1)
    value_own = lax.dynamic_slice_in_dim(values, kv_head * HD, HD, 1)
    paired = jnp.concatenate([key_own, value_own], axis=1)
    padded = with_halo(paired, (("sp", 0),), WINDOW)
    blocks = tok_dev // WINDOW
    framed = padded.reshape(blocks + 2, WINDOW, 2 * HD)
    banded = jnp.concatenate([framed[:-2], framed[1:-1], framed[2:]], axis=1)
    key_band = banded[:, :, :HD]
    value_band = banded[:, :, HD:]
    query_blocks = queries.reshape(blocks, WINDOW, heads_dev, HD)
    scores = jnp.einsum(
        "nqhd,njd->nhqj", query_blocks, key_band, preferred_element_type=jnp.float32
    ) * HD ** (-0.5)
    offset = sp_idx * tok_dev
    seq_total = tok_dev * n_sp
    query_pos = (
        offset + jnp.arange(blocks)[:, None, None] * WINDOW + jnp.arange(WINDOW)[None, :, None]
    )
    key_pos = (
        offset
        - WINDOW
        + jnp.arange(blocks)[:, None, None] * WINDOW
        + jnp.arange(3 * WINDOW)[None, None, :]
    )
    allowed = (jnp.abs(query_pos - key_pos) <= WINDOW) & (key_pos >= 0) & (key_pos < seq_total)
    scores = jnp.where(allowed[:, None], scores, -jnp.inf)
    sink_level = sink.reshape(1, heads_dev, 1, 1)
    row_peak = jnp.maximum(scores.max(-1, keepdims=True), sink_level)
    probabilities = jnp.exp(scores - row_peak)
    denominator = probabilities.sum(-1, keepdims=True) + jnp.exp(sink_level - row_peak)
    weights = (probabilities / denominator).astype(jnp.bfloat16)
    attended = jnp.einsum("nhqj,njd->nqhd", weights, value_band, preferred_element_type=jnp.float32)
    return attended.astype(jnp.bfloat16).reshape(tok_dev, heads_dev * HD)


def local_general(
    queries,
    keys,
    values,
    sink,
    w_out,
    stream,
    gain,
    routes,
    route_weights,
    w_gate,
    w_up,
    w_down,
    shared_gate,
    shared_up,
    shared_down,
):
    tok_dev = queries.shape[0]
    n_tp = lax.axis_size("tp")
    n_sp = lax.axis_size("sp")
    tp_idx = lax.axis_index("tp")
    attended = attention(queries, keys, values, sink)
    rows_dev = tok_dev // n_tp
    d_dev = w_down.shape[2]
    projected = lax.psum_scatter(
        jnp.dot(attended, w_out, preferred_element_type=jnp.float32),
        "tp",
        scatter_dimension=0,
        tiled=True,
    )
    mixed_rows = (stream.astype(jnp.float32) + projected).astype(jnp.bfloat16)
    whole_rows = lax.all_gather(mixed_rows, "tp", axis=0, tiled=True)
    wide_rows = whole_rows.astype(jnp.float32)
    scale_rows = lax.rsqrt(jnp.mean(wide_rows * wide_rows, axis=-1, keepdims=True) + NORM_EPS)
    normed = (wide_rows * scale_rows * gain.astype(jnp.float32)).astype(jnp.bfloat16)
    residual = lax.dynamic_slice_in_dim(wide_rows, tp_idx * d_dev, d_dev, 1)
    exp_dev = w_gate.shape[0]
    capacity = max(1, 2 * tok_dev * TOPK // (n_tp * EXPERTS))
    slot_count = EXPERTS * capacity
    blocked_routes = routes.reshape(n_tp, rows_dev, TOPK)
    destination = jax.vmap(lambda block_routes: slot_ids(block_routes, capacity))(blocked_routes)
    slot_select = destination[:, None, :] == jnp.arange(slot_count)[None, :, None]
    slot_select = slot_select.reshape(n_tp, slot_count, rows_dev, TOPK).astype(jnp.float32)
    dispatch_table = jnp.sum(slot_select, axis=-1).astype(jnp.bfloat16)
    combine_table = jnp.sum(slot_select * route_weights.reshape(n_tp, 1, rows_dev, TOPK), axis=-1)
    normed_blocks = normed.reshape(n_tp, rows_dev, D)
    own_table = lax.dynamic_index_in_dim(dispatch_table, tp_idx, 0, keepdims=False)
    own_rows = lax.dynamic_index_in_dim(normed_blocks, tp_idx, 0, keepdims=False)
    outgoing = jnp.dot(own_table, own_rows, preferred_element_type=jnp.float32).astype(jnp.bfloat16)
    arrived = lax.all_to_all(outgoing, "sp", split_axis=0, concat_axis=0, tiled=True)
    arrived = arrived.reshape(1, n_sp, exp_dev, capacity, D)
    piece_rows = lax.all_gather(arrived, "tp", axis=0, tiled=True)
    gate_act = jnp.einsum(
        "tsecd,efd->tsecf", piece_rows, w_gate, preferred_element_type=jnp.float32
    )
    up_act = jnp.einsum("tsecd,efd->tsecf", piece_rows, w_up, preferred_element_type=jnp.float32)
    hidden = (jax.nn.silu(gate_act) * up_act).astype(jnp.bfloat16)
    shared_gate_act = jnp.einsum(
        "td,fd->tf", normed, shared_gate, preferred_element_type=jnp.float32
    )
    shared_up_act = jnp.einsum("td,fd->tf", normed, shared_up, preferred_element_type=jnp.float32)
    shared_hidden = (jax.nn.silu(shared_gate_act) * shared_up_act).astype(jnp.bfloat16)
    shared_hidden = shared_hidden.reshape(1, 1, 1, tok_dev, shared_hidden.shape[1])
    expert_piece = lax.all_gather(hidden, "tp", axis=4, tiled=True)
    shared_piece = lax.all_gather(shared_hidden, "tp", axis=4, tiled=True)
    piece_width = expert_piece.shape[4]
    routed_total = jnp.einsum(
        "tsecf,efd->tsecd", expert_piece, w_down, preferred_element_type=jnp.float32
    )
    shared_total = jnp.dot(
        shared_piece.reshape(tok_dev, piece_width), shared_down, preferred_element_type=jnp.float32
    )
    returned = lax.all_to_all(
        routed_total.astype(jnp.bfloat16), "sp", split_axis=1, concat_axis=1, tiled=True
    )
    returned = returned.reshape(n_tp, slot_count, d_dev).astype(jnp.float32)
    routed = jnp.einsum("tmr,tmd->trd", combine_table, returned, precision=lax.Precision.HIGHEST)
    routed = routed.reshape(tok_dev, d_dev)
    return (residual + routed + shared_total).astype(jnp.bfloat16)


def in_vmem(a):
    return pltpu.with_memory_space_constraint(a, pltpu.MemorySpace.VMEM)


NT = (((1,), (1,)), ((), ()))


def silu_product(gate, up):
    return (gate / (1.0 + jnp.exp(-gate)) * up).astype(jnp.bfloat16)


def spots(rows, shape, where_ref, axis):
    quad = lax.broadcasted_iota(jnp.int32, shape, axis) // rows
    return jnp.bitwise_xor(quad, where_ref[1])


def up_kernel(where_ref, *refs, places, count, own, exp_dev, capacity, quads, rows):
    pieces_hbm = refs[:count]
    gate_hbm, up_hbm = refs[count : count + 2]
    rest = refs[count + 2 :]
    pieces, piece_sems = rest[-2:]
    rest = rest[:-2]
    piece_copies = [
        pltpu.make_async_copy(ref, pieces.at[i], piece_sems.at[i])
        for i, ref in enumerate(pieces_hbm)
    ]
    for copy in piece_copies:
        copy.start()
    shared_copies = []
    if own:
        shared_hbm, rest = rest[:2], rest[2:]
        sgate_ref, sup_ref, shared_sems = rest[-3:]
        rest = rest[:-3]
        for i, ref in enumerate((sgate_ref, sup_ref)):
            shared_copies.append(pltpu.make_async_copy(shared_hbm[i], ref, shared_sems.at[i]))
            shared_copies[-1].start()
    hidden_ref, table_ref = rest[:2]
    weights_ref, slots_ref, sems = rest[-3:]
    piece = gate_hbm.shape[1]
    copies = []
    for e in range(exp_dev):
        copies.append(
            (
                pltpu.make_async_copy(gate_hbm.at[e], weights_ref.at[e, :piece], sems.at[0, e]),
                pltpu.make_async_copy(up_hbm.at[e], weights_ref.at[e, piece:], sems.at[1, e]),
            )
        )
    for e in range(min(AHEAD, exp_dev)):
        for copy in copies[e]:
            copy.start()

    width = quads * capacity
    lanes = exp_dev * width
    tokens = quads * rows

    def slot(shape, axis):
        index = lax.broadcasted_iota(jnp.int32, shape, axis)
        return index // width, (index // capacity) % quads, index % capacity

    column = lax.broadcasted_iota(jnp.int32, (lanes, 2 * EXPERTS), 1)
    expert = slot((lanes, 2 * EXPERTS), 0)[0] + where_ref[0]
    of_rank = (column == expert).astype(jnp.float32).astype(jnp.bfloat16)
    of_weight = (column == expert + EXPERTS).astype(jnp.float32).astype(jnp.bfloat16)

    def wanted(axis):
        shape = (lanes, tokens) if axis == 0 else (tokens, lanes)
        _, spot, rank = slot(shape, axis)
        same = spot == spots(rows, shape, where_ref, 1 - axis)
        return jnp.where(same, rank + 1, -1).astype(jnp.float32)

    by_slot, by_token = wanted(0), wanted(1)
    for unit, members in enumerate(places):
        for ref in members:
            piece_copies[ref].wait()
        extra = jnp.concatenate([pieces[ref, :, D:] for ref in members], axis=0)
        held = jnp.concatenate([pieces[ref, :, :D] for ref in members], axis=0)
        ranks = lax.dot_general(of_rank, extra, NT, preferred_element_type=jnp.float32)
        table = jnp.where(ranks == by_slot, 1.0, 0.0).astype(jnp.bfloat16)
        picked = jnp.dot(table, held, preferred_element_type=jnp.float32).astype(jnp.bfloat16)
        for e in range(exp_dev):
            slots_ref[e, unit * width : (unit + 1) * width, :] = picked[e * width : (e + 1) * width]
        ranks = lax.dot_general(extra, of_rank, NT, preferred_element_type=jnp.float32)
        weights = lax.dot_general(extra, of_weight, NT, preferred_element_type=jnp.float32)
        table = jnp.where(ranks == by_token, weights, 0.0).astype(jnp.bfloat16)
        for quad in range(quads):
            start = pl.multiple_of(jnp.bitwise_xor(where_ref[1], quad) * rows, rows)
            table_ref[unit, pl.ds(start, rows), :] = table[quad * rows : (quad + 1) * rows]
        if own and unit == 0:
            for copy in shared_copies:
                copy.wait()
            gate = lax.dot_general(held, sgate_ref[...], NT, preferred_element_type=jnp.float32)
            up = lax.dot_general(held, sup_ref[...], NT, preferred_element_type=jnp.float32)
            hidden = silu_product(gate, up)
            for quad in range(quads):
                start = jnp.bitwise_xor(where_ref[1], quad) * rows
                tall = hidden_ref.shape[1]
                hidden_ref[
                    exp_dev + start // tall, pl.ds(pl.multiple_of(start % tall, rows), rows), :
                ] = hidden[quad * rows : (quad + 1) * rows]
    for e in range(exp_dev):
        for copy in copies[e]:
            copy.wait()
        if e + AHEAD < exp_dev:
            for copy in copies[e + AHEAD]:
                copy.start()
        held = slots_ref[e]
        both = lax.dot_general(held, weights_ref[e], NT, preferred_element_type=jnp.float32)
        hidden_ref[e] = silu_product(both[:, :piece], both[:, piece:])


def down_kernel(where_ref, *refs, own, units, quads, exp_dev, capacity, piece):
    hiddens = refs[:quads]
    table_ref, down_hbm = refs[quads : quads + 2]
    rest = refs[quads + 2 :]
    if own:
        sdown_hbm, shared_ref = rest[:2]
        sdown_ref, shared_sem = rest[-2:]
        rest = rest[2:]
        shared_copy = pltpu.make_async_copy(sdown_hbm, sdown_ref, shared_sem)
        shared_copy.start()
    outs = rest[:units]
    downs, result_ref, sems = rest[units:][:3]
    copies = [
        pltpu.make_async_copy(down_hbm.at[e], downs.at[e], sems.at[e]) for e in range(exp_dev)
    ]
    for copy in copies[:DOWN_AHEAD]:
        copy.start()
    width = quads * capacity

    def product(parts, weight_ref, lead):
        total = None
        for quad, part in enumerate(parts):
            start = pl.multiple_of(jnp.bitwise_xor(where_ref[1], quad) * piece, piece)
            weight = weight_ref[lead + (pl.ds(start, piece), slice(None))]
            term = jnp.dot(part, weight, preferred_element_type=jnp.float32)
            total = term if total is None else total + term
        return total

    if own:
        shared_copy.wait()
        tall = hiddens[0].shape[1]
        for part in range(shared_ref.shape[0] // tall):
            shared_ref[part * tall : (part + 1) * tall] = product(
                [ref[exp_dev + part] for ref in hiddens], sdown_ref, ()
            )
    for e in range(exp_dev):
        copies[e].wait()
        if e + DOWN_AHEAD < exp_dev:
            copies[e + DOWN_AHEAD].start()
        total = product([ref[e] for ref in hiddens], downs, (e,)).astype(jnp.bfloat16)
        for unit in range(units):
            result_ref[unit, e * width : (e + 1) * width, :] = total[
                unit * width : (unit + 1) * width
            ]
    for unit in range(units):
        routed = jnp.dot(table_ref[unit], result_ref[unit], preferred_element_type=jnp.float32)
        outs[unit][...] = routed.astype(jnp.bfloat16)


def local_torus(
    queries,
    keys,
    values,
    sink,
    w_out,
    stream,
    gain,
    routes,
    route_weights,
    w_gate,
    w_up,
    w_down,
    shared_gate,
    shared_up,
    shared_down,
    *,
    nx,
):
    tok_dev = queries.shape[0]
    n_tp = lax.axis_size("tp")
    n_sp = lax.axis_size("sp")
    nz = n_sp // nx
    tp_idx = lax.axis_index("tp")
    sp_idx = lax.axis_index("sp")
    rows = tok_dev // n_tp
    d_dev = w_down.shape[2]
    exp_dev = w_gate.shape[0]
    piece = w_gate.shape[1]
    capacity = max(1, 2 * tok_dev * TOPK // (n_tp * EXPERTS))
    bf16, f32 = jnp.bfloat16, jnp.float32

    def swap(a, axis, bit):
        pairs = [(i, i ^ bit) for i in range(lax.axis_size(axis))]
        return lax.ppermute(a, axis, pairs)

    def core_swap(a):
        return swap(a, "tp", 1)

    def y_swap(a):
        return swap(a, "tp", 2)

    def x_swap(a):
        return swap(a, "sp", 1)

    def z_swap(a, bit):
        return swap(a, "sp", bit * nx)

    own_routes = lax.dynamic_slice_in_dim(routes, tp_idx * rows, rows, 0)
    own_weights = lax.dynamic_slice_in_dim(route_weights, tp_idx * rows, rows, 0)
    hits = own_routes[:, :, None] == jnp.arange(EXPERTS)[None, None, :]
    named = jnp.any(hits, axis=1)
    not_later = (jnp.arange(rows)[:, None] >= jnp.arange(rows)[None, :]).astype(bf16)
    ranks = jnp.dot(not_later, named.astype(bf16), preferred_element_type=f32)
    extra = jnp.concatenate(
        [
            jnp.where(named, ranks, 0.0),
            jnp.sum(jnp.where(hits, own_weights[:, :, None], 0.0), axis=1),
        ],
        axis=1,
    ).astype(bf16)

    attended = attention(queries, keys, values, sink)
    projected = jnp.dot(attended, w_out, preferred_element_type=f32)
    quarters = projected.reshape(n_tp // 2, 2, rows, D)
    core = tp_idx % 2
    own_y = tp_idx // 2
    keep = lax.dynamic_index_in_dim(quarters, core, 1, keepdims=False)
    give = lax.dynamic_index_in_dim(quarters, 1 - core, 1, keepdims=False)
    chip = keep + core_swap(give.astype(bf16)).astype(f32)
    away = lax.dynamic_index_in_dim(chip, 1 - own_y, 0, keepdims=False).astype(bf16)
    home = lax.dynamic_index_in_dim(chip, own_y, 0, keepdims=False)
    summed = home + y_swap(away).astype(f32)
    mixed = (stream.astype(f32) + summed).astype(bf16)
    wide = mixed.astype(f32)
    scale = lax.rsqrt(jnp.mean(wide * wide, axis=-1, keepdims=True) + NORM_EPS)
    normed = (wide * scale * gain.astype(f32)).astype(bf16)
    own = jnp.concatenate([normed, extra], axis=1)

    chunk_z = nz // 2
    far = [own, z_swap(own, 1), z_swap(own, 2)]
    far.append(z_swap(far[2], 1))
    chunks = [([], []), ([], [])]
    for k in range(nz):
        operands, places = chunks[1 - k // chunk_z]
        by_x, by_y = x_swap(far[k]), y_swap(far[k])
        both = y_swap(by_x) if k in (1, 2) else x_swap(by_y)
        base = len(operands)
        for rows_in in (far[k], by_y, by_x, both):
            operands += [rows_in, core_swap(rows_in)]
        places += [range(base, base + n_tp), range(base + n_tp, base + 2 * n_tp)]
    quads = n_tp

    def columns(a, index, width):
        return lax.dynamic_slice_in_dim(a, index * width, width, 1)

    half = 2 * d_dev
    near_y = columns(mixed, own_y, half)
    far_y = y_swap(columns(mixed, 1 - own_y, half))
    by_y = jnp.concatenate([near_y, far_y], axis=0)
    here = columns(by_y, core, d_dev)
    there = core_swap(columns(by_y, 1 - core, d_dev))
    both = jnp.stack([here[:rows], there[:rows], here[rows:], there[rows:]], axis=0)
    residual = jnp.take(both, jnp.arange(n_tp) ^ tp_idx, axis=0).reshape(tok_dev, d_dev)

    where = jnp.stack([sp_idx * exp_dev, tp_idx]).astype(jnp.int32)
    width = quads * capacity
    lanes = exp_dev * width
    smem = pl.BlockSpec(memory_space=pltpu.SMEM)
    vmem = pl.BlockSpec(memory_space=pltpu.VMEM)
    hbm = pl.BlockSpec(memory_space=pltpu.MemorySpace.HBM)

    def in_hbm(*arrays):
        return [pltpu.with_memory_space_constraint(a, pltpu.MemorySpace.HBM) for a in arrays]

    def up_call(operands, places, own):
        units = len(places)
        shared = [shared_gate, shared_up] if own else []
        kernel = functools.partial(
            up_kernel,
            places=places,
            count=len(operands),
            own=own,
            exp_dev=exp_dev,
            capacity=capacity,
            quads=quads,
            rows=rows,
        )
        groups = exp_dev + (tok_dev // (units * width) if own else 0)
        out_shape = [
            jax.ShapeDtypeStruct((groups, units * width, piece), bf16),
            jax.ShapeDtypeStruct((units, tok_dev, lanes), bf16),
        ]
        return pl.pallas_call(
            kernel,
            in_specs=[smem] + [hbm] * (len(operands) + 2 + len(shared)),
            out_specs=[vmem] * len(out_shape),
            out_shape=out_shape,
            scratch_shapes=[
                pltpu.VMEM((exp_dev, 2 * piece, D), bf16),
                pltpu.VMEM((exp_dev, units * width, D), bf16),
                pltpu.SemaphoreType.DMA((2, exp_dev)),
            ]
            + [pltpu.VMEM((piece, D), bf16)] * len(shared)
            + [pltpu.SemaphoreType.DMA((2,))] * (len(shared) // 2)
            + [
                pltpu.VMEM((len(operands), rows, D + LANES), bf16),
                pltpu.SemaphoreType.DMA((len(operands),)),
            ],
            compiler_params=pltpu.CompilerParams(vmem_limit_bytes=UP_VMEM),
            name="up_kernel",
        )(where, *in_hbm(*operands, w_gate, w_up, *shared))

    def down_call(hiddens, table, own):
        units = table.shape[0]
        kernel = functools.partial(
            down_kernel,
            own=own,
            units=units,
            quads=quads,
            exp_dev=exp_dev,
            capacity=capacity,
            piece=piece,
        )
        out_shape = [jax.ShapeDtypeStruct((tok_dev, d_dev), bf16)] * units
        more = []
        if own:
            out_shape = [jax.ShapeDtypeStruct((tok_dev, d_dev), f32)] + out_shape
            more = [shared_down]
        return pl.pallas_call(
            kernel,
            in_specs=[smem] + [vmem] * (quads + 1) + [hbm] * (1 + len(more)),
            out_specs=[vmem] * len(out_shape),
            out_shape=out_shape,
            scratch_shapes=[
                pltpu.VMEM((exp_dev, quads * piece, d_dev), bf16),
                pltpu.VMEM((units, lanes, d_dev), bf16),
                pltpu.SemaphoreType.DMA((exp_dev,)),
            ]
            + [pltpu.VMEM((quads * piece, d_dev), bf16), pltpu.SemaphoreType.DMA] * len(more),
            compiler_params=pltpu.CompilerParams(vmem_limit_bytes=DOWN_VMEM),
            name="down_kernel",
        )(where, *map(in_vmem, hiddens), table, *in_hbm(w_down, *more))

    total = residual.astype(f32)
    sums = {}
    for chunk, (operands, places) in enumerate(chunks):
        hidden, table = up_call(operands, places, chunk == 1)
        by_y = y_swap(hidden)
        hiddens = [hidden, core_swap(hidden)]
        hiddens += [by_y, core_swap(by_y)]
        parts = list(down_call(hiddens, table, chunk == 1))
        if chunk == 1:
            total += parts.pop(0)
        for pair in range(chunk_z):
            k = (1 - chunk) * chunk_z + pair
            there = x_swap(parts[pair * nx + 1])
            sums[k] = parts[pair * nx].astype(f32) + there.astype(f32)
    from_next = z_swap(sums[3].astype(bf16), 1)
    from_far = z_swap((sums[2] + from_next.astype(f32)).astype(bf16), 2)
    total += sums[0] + z_swap(sums[1].astype(bf16), 1).astype(f32)
    return (total + from_far.astype(f32)).astype(bf16)


def solution(mesh):
    placed = (
        P("sp", "tp"),
        P("sp", None),
        P("sp", None),
        P("tp"),
        P("tp", None),
        P(("sp", "tp"), None),
        P(),
        P("sp", None),
        P("sp", None),
        P("sp", "tp", None),
        P("sp", "tp", None),
        P("sp", None, "tp"),
        P("tp", None),
        P("tp", None),
        P(None, "tp"),
    )
    n_sp, n_tp = mesh.shape["sp"], mesh.shape["tp"]
    nx = 1
    while 4 * nx * nx <= n_sp:
        nx *= 2

    pairs = nx == 2 and n_tp == 4 and n_sp == nx * 4

    def local(*args):
        tok_dev, piece = args[0].shape[0], args[9].shape[1]
        capacity = 2 * tok_dev * TOPK // (n_tp * EXPERTS)
        tiles = capacity % 8 == 0 and piece % LANES == 0 and (tok_dev // n_tp) % 16 == 0
        slots = n_sp * n_tp * capacity == tok_dev
        if pairs and tiles and slots:
            return local_torus(*args, nx=nx)
        return local_general(*args)

    return jax.shard_map(
        local, mesh=mesh, in_specs=placed, out_specs=P("sp", "tp"), check_vma=False
    )
```

```python
import functools

import jax
import jax.numpy as jnp
from jax import lax
from jax.experimental import pallas as pl
from jax.experimental.pallas import tpu as pltpu
from jax.sharding import PartitionSpec as P


D = 2048
HEADS = 16
KV_HEADS = 4
HD = 64
WINDOW = 128
EXPERTS = 64
TOPK = 4


NORM_EPS = 1e-05
LANES = 128
AHEAD = 2
RING = AHEAD + 1
DOWN_AHEAD = 4
UP_VMEM = 24 * 1024 * 1024
DOWN_VMEM = 20 * 1024 * 1024


def with_halo(array, sides, width):
    for axis, dim in sides:
        devices, length = (lax.axis_size(axis), array.shape[dim])
        up = [(i, (i + 1) % devices) for i in range(devices - 1)]
        down = [(j, i) for i, j in up]
        last = lax.slice_in_dim(array, length - width, length, axis=dim)
        leading = lax.slice_in_dim(array, 0, width, axis=dim)
        before = lax.ppermute(last, axis, up)
        after = lax.ppermute(leading, axis, down)
        array = jnp.concatenate([before, array, after], axis=dim)
    return array


def slot_ids(block_routes, capacity):
    flat_routes = block_routes.reshape(-1)
    hit_table = (flat_routes[:, None] == jnp.arange(EXPERTS)[None, :]).astype(jnp.int32)
    earlier = jnp.cumsum(hit_table, axis=0) - hit_table
    slot_rank = jnp.sum(earlier * hit_table, axis=1)
    return flat_routes * capacity + slot_rank


def attention(queries, keys, values, sink):
    tok_dev = queries.shape[0]
    n_tp = lax.axis_size("tp")
    n_sp = lax.axis_size("sp")
    tp_idx = lax.axis_index("tp")
    sp_idx = lax.axis_index("sp")
    heads_dev = HEADS // n_tp
    group = HEADS // KV_HEADS
    kv_head = tp_idx * heads_dev // group
    key_own = lax.dynamic_slice_in_dim(keys, kv_head * HD, HD, 1)
    value_own = lax.dynamic_slice_in_dim(values, kv_head * HD, HD, 1)
    paired = jnp.concatenate([key_own, value_own], axis=1)
    padded = with_halo(paired, (("sp", 0),), WINDOW)
    blocks = tok_dev // WINDOW
    framed = padded.reshape(blocks + 2, WINDOW, 2 * HD)
    banded = jnp.concatenate([framed[:-2], framed[1:-1], framed[2:]], axis=1)
    key_band = banded[:, :, :HD]
    value_band = banded[:, :, HD:]
    query_blocks = queries.reshape(blocks, WINDOW, heads_dev, HD)
    scores = jnp.einsum(
        "nqhd,njd->nhqj", query_blocks, key_band, preferred_element_type=jnp.float32
    ) * HD ** (-0.5)
    offset = sp_idx * tok_dev
    seq_total = tok_dev * n_sp
    query_pos = (
        offset + jnp.arange(blocks)[:, None, None] * WINDOW + jnp.arange(WINDOW)[None, :, None]
    )
    key_pos = (
        offset
        - WINDOW
        + jnp.arange(blocks)[:, None, None] * WINDOW
        + jnp.arange(3 * WINDOW)[None, None, :]
    )
    allowed = (jnp.abs(query_pos - key_pos) <= WINDOW) & (key_pos >= 0) & (key_pos < seq_total)
    scores = jnp.where(allowed[:, None], scores, -jnp.inf)
    sink_level = sink.reshape(1, heads_dev, 1, 1)
    row_peak = jnp.maximum(scores.max(-1, keepdims=True), sink_level)
    probabilities = jnp.exp(scores - row_peak)
    denominator = probabilities.sum(-1, keepdims=True) + jnp.exp(sink_level - row_peak)
    weights = (probabilities / denominator).astype(jnp.bfloat16)
    attended = jnp.einsum("nhqj,njd->nqhd", weights, value_band, preferred_element_type=jnp.float32)
    return attended.astype(jnp.bfloat16).reshape(tok_dev, heads_dev * HD)


def local_general(
    queries,
    keys,
    values,
    sink,
    w_out,
    stream,
    gain,
    routes,
    route_weights,
    w_gate,
    w_up,
    w_down,
    shared_gate,
    shared_up,
    shared_down,
):
    tok_dev = queries.shape[0]
    n_tp = lax.axis_size("tp")
    n_sp = lax.axis_size("sp")
    tp_idx = lax.axis_index("tp")
    attended = attention(queries, keys, values, sink)
    rows_dev = tok_dev // n_tp
    d_dev = w_down.shape[2]
    projected = lax.psum_scatter(
        jnp.dot(attended, w_out, preferred_element_type=jnp.float32),
        "tp",
        scatter_dimension=0,
        tiled=True,
    )
    mixed_rows = (stream.astype(jnp.float32) + projected).astype(jnp.bfloat16)
    whole_rows = lax.all_gather(mixed_rows, "tp", axis=0, tiled=True)
    wide_rows = whole_rows.astype(jnp.float32)
    scale_rows = lax.rsqrt(jnp.mean(wide_rows * wide_rows, axis=-1, keepdims=True) + NORM_EPS)
    normed = (wide_rows * scale_rows * gain.astype(jnp.float32)).astype(jnp.bfloat16)
    residual = lax.dynamic_slice_in_dim(wide_rows, tp_idx * d_dev, d_dev, 1)
    exp_dev = w_gate.shape[0]
    capacity = max(1, 2 * tok_dev * TOPK // (n_tp * EXPERTS))
    slot_count = EXPERTS * capacity
    blocked_routes = routes.reshape(n_tp, rows_dev, TOPK)
    destination = jax.vmap(lambda block_routes: slot_ids(block_routes, capacity))(blocked_routes)
    slot_select = destination[:, None, :] == jnp.arange(slot_count)[None, :, None]
    slot_select = slot_select.reshape(n_tp, slot_count, rows_dev, TOPK).astype(jnp.float32)
    dispatch_table = jnp.sum(slot_select, axis=-1).astype(jnp.bfloat16)
    combine_table = jnp.sum(slot_select * route_weights.reshape(n_tp, 1, rows_dev, TOPK), axis=-1)
    normed_blocks = normed.reshape(n_tp, rows_dev, D)
    own_table = lax.dynamic_index_in_dim(dispatch_table, tp_idx, 0, keepdims=False)
    own_rows = lax.dynamic_index_in_dim(normed_blocks, tp_idx, 0, keepdims=False)
    outgoing = jnp.dot(own_table, own_rows, preferred_element_type=jnp.float32).astype(jnp.bfloat16)
    arrived = lax.all_to_all(outgoing, "sp", split_axis=0, concat_axis=0, tiled=True)
    arrived = arrived.reshape(1, n_sp, exp_dev, capacity, D)
    piece_rows = lax.all_gather(arrived, "tp", axis=0, tiled=True)
    gate_act = jnp.einsum(
        "tsecd,efd->tsecf", piece_rows, w_gate, preferred_element_type=jnp.float32
    )
    up_act = jnp.einsum("tsecd,efd->tsecf", piece_rows, w_up, preferred_element_type=jnp.float32)
    hidden = (jax.nn.silu(gate_act) * up_act).astype(jnp.bfloat16)
    shared_gate_act = jnp.einsum(
        "td,fd->tf", normed, shared_gate, preferred_element_type=jnp.float32
    )
    shared_up_act = jnp.einsum("td,fd->tf", normed, shared_up, preferred_element_type=jnp.float32)
    shared_hidden = (jax.nn.silu(shared_gate_act) * shared_up_act).astype(jnp.bfloat16)
    shared_hidden = shared_hidden.reshape(1, 1, 1, tok_dev, shared_hidden.shape[1])
    expert_piece = lax.all_gather(hidden, "tp", axis=4, tiled=True)
    shared_piece = lax.all_gather(shared_hidden, "tp", axis=4, tiled=True)
    piece_width = expert_piece.shape[4]
    routed_total = jnp.einsum(
        "tsecf,efd->tsecd", expert_piece, w_down, preferred_element_type=jnp.float32
    )
    shared_total = jnp.dot(
        shared_piece.reshape(tok_dev, piece_width), shared_down, preferred_element_type=jnp.float32
    )
    returned = lax.all_to_all(
        routed_total.astype(jnp.bfloat16), "sp", split_axis=1, concat_axis=1, tiled=True
    )
    returned = returned.reshape(n_tp, slot_count, d_dev).astype(jnp.float32)
    routed = jnp.einsum("tmr,tmd->trd", combine_table, returned, precision=lax.Precision.HIGHEST)
    routed = routed.reshape(tok_dev, d_dev)
    return (residual + routed + shared_total).astype(jnp.bfloat16)


def in_vmem(a):
    return pltpu.with_memory_space_constraint(a, pltpu.MemorySpace.VMEM)


NT = (((1,), (1,)), ((), ()))


def silu_product(gate, up):
    return (gate / (1.0 + jnp.exp(-gate)) * up).astype(jnp.bfloat16)


def spots(rows, shape, where_ref, axis):
    quad = lax.broadcasted_iota(jnp.int32, shape, axis) // rows
    return jnp.bitwise_xor(quad, where_ref[1])


def up_kernel(where_ref, *refs, places, count, own, exp_dev, capacity, quads, rows):
    pieces_hbm = refs[:count]
    gate_hbm, up_hbm = refs[count : count + 2]
    rest = refs[count + 2 :]
    pieces, piece_sems = rest[-2:]
    rest = rest[:-2]
    piece_copies = [
        pltpu.make_async_copy(ref, pieces.at[i], piece_sems.at[i])
        for i, ref in enumerate(pieces_hbm)
    ]
    for copy in piece_copies:
        copy.start()
    shared_copies = []
    if own:
        shared_hbm, rest = rest[:2], rest[2:]
        sgate_ref, sup_ref, shared_sems = rest[-3:]
        rest = rest[:-3]
        for i, ref in enumerate((sgate_ref, sup_ref)):
            shared_copies.append(pltpu.make_async_copy(shared_hbm[i], ref, shared_sems.at[i]))
            shared_copies[-1].start()
    hidden_ref, table_ref = rest[:2]
    weights_ref, slots_ref, sems = rest[-3:]
    piece = gate_hbm.shape[1]
    copies = []
    for e in range(exp_dev):
        copies.append(
            (
                pltpu.make_async_copy(gate_hbm.at[e], weights_ref.at[e % RING, :piece], sems.at[0, e]),
                pltpu.make_async_copy(up_hbm.at[e], weights_ref.at[e % RING, piece:], sems.at[1, e]),
            )
        )
    for e in range(min(AHEAD, exp_dev)):
        for copy in copies[e]:
            copy.start()

    width = quads * capacity
    lanes = exp_dev * width
    tokens = quads * rows

    def slot(shape, axis):
        index = lax.broadcasted_iota(jnp.int32, shape, axis)
        return index // width, (index // capacity) % quads, index % capacity

    column = lax.broadcasted_iota(jnp.int32, (lanes, 2 * EXPERTS), 1)
    expert = slot((lanes, 2 * EXPERTS), 0)[0] + where_ref[0]
    of_rank = (column == expert).astype(jnp.float32).astype(jnp.bfloat16)
    of_weight = (column == expert + EXPERTS).astype(jnp.float32).astype(jnp.bfloat16)

    def wanted(axis):
        shape = (lanes, tokens) if axis == 0 else (tokens, lanes)
        _, spot, rank = slot(shape, axis)
        same = spot == spots(rows, shape, where_ref, 1 - axis)
        return jnp.where(same, rank + 1, -1).astype(jnp.float32)

    by_slot, by_token = wanted(0), wanted(1)
    for unit, members in enumerate(places):
        for ref in members:
            piece_copies[ref].wait()
        extra = jnp.concatenate([pieces[ref, :, D:] for ref in members], axis=0)
        held = jnp.concatenate([pieces[ref, :, :D] for ref in members], axis=0)
        ranks = lax.dot_general(of_rank, extra, NT, preferred_element_type=jnp.float32)
        table = jnp.where(ranks == by_slot, 1.0, 0.0).astype(jnp.bfloat16)
        picked = jnp.dot(table, held, preferred_element_type=jnp.float32).astype(jnp.bfloat16)
        for e in range(exp_dev):
            slots_ref[e, unit * width : (unit + 1) * width, :] = picked[e * width : (e + 1) * width]
        ranks = lax.dot_general(extra, of_rank, NT, preferred_element_type=jnp.float32)
        weights = lax.dot_general(extra, of_weight, NT, preferred_element_type=jnp.float32)
        table = jnp.where(ranks == by_token, weights, 0.0).astype(jnp.bfloat16)
        for quad in range(quads):
            start = pl.multiple_of(jnp.bitwise_xor(where_ref[1], quad) * rows, rows)
            table_ref[unit, pl.ds(start, rows), :] = table[quad * rows : (quad + 1) * rows]
        if own and unit == 0:
            for copy in shared_copies:
                copy.wait()
            gate = lax.dot_general(held, sgate_ref[...], NT, preferred_element_type=jnp.float32)
            up = lax.dot_general(held, sup_ref[...], NT, preferred_element_type=jnp.float32)
            hidden = silu_product(gate, up)
            for quad in range(quads):
                start = jnp.bitwise_xor(where_ref[1], quad) * rows
                tall = hidden_ref.shape[1]
                hidden_ref[
                    exp_dev + start // tall, pl.ds(pl.multiple_of(start % tall, rows), rows), :
                ] = hidden[quad * rows : (quad + 1) * rows]
    for e in range(exp_dev):
        for copy in copies[e]:
            copy.wait()
        if e + AHEAD < exp_dev:
            for copy in copies[e + AHEAD]:
                copy.start()
        held = slots_ref[e]
        both = lax.dot_general(held, weights_ref[e % RING], NT, preferred_element_type=jnp.float32)
        hidden_ref[e] = silu_product(both[:, :piece], both[:, piece:])


def down_kernel(where_ref, *refs, own, units, quads, exp_dev, capacity, piece):
    hiddens = refs[:quads]
    table_ref, down_hbm = refs[quads : quads + 2]
    rest = refs[quads + 2 :]
    if own:
        sdown_hbm, shared_ref = rest[:2]
        sdown_ref, shared_sem = rest[-2:]
        rest = rest[2:]
        shared_copy = pltpu.make_async_copy(sdown_hbm, sdown_ref, shared_sem)
        shared_copy.start()
    outs = rest[:units]
    downs, result_ref, sems = rest[units:][:3]
    copies = [
        pltpu.make_async_copy(down_hbm.at[e], downs.at[e], sems.at[e]) for e in range(exp_dev)
    ]
    for copy in copies[:DOWN_AHEAD]:
        copy.start()
    width = quads * capacity

    def product(parts, weight_ref, lead):
        total = None
        for quad, part in enumerate(parts):
            start = pl.multiple_of(jnp.bitwise_xor(where_ref[1], quad) * piece, piece)
            weight = weight_ref[lead + (pl.ds(start, piece), slice(None))]
            term = jnp.dot(part, weight, preferred_element_type=jnp.float32)
            total = term if total is None else total + term
        return total

    if own:
        shared_copy.wait()
        tall = hiddens[0].shape[1]
        for part in range(shared_ref.shape[0] // tall):
            shared_ref[part * tall : (part + 1) * tall] = product(
                [ref[exp_dev + part] for ref in hiddens], sdown_ref, ()
            )
    for e in range(exp_dev):
        copies[e].wait()
        if e + DOWN_AHEAD < exp_dev:
            copies[e + DOWN_AHEAD].start()
        total = product([ref[e] for ref in hiddens], downs, (e,)).astype(jnp.bfloat16)
        for unit in range(units):
            result_ref[unit, e * width : (e + 1) * width, :] = total[
                unit * width : (unit + 1) * width
            ]
    for unit in range(units):
        routed = jnp.dot(table_ref[unit], result_ref[unit], preferred_element_type=jnp.float32)
        outs[unit][...] = routed.astype(jnp.bfloat16)


def local_torus(
    queries,
    keys,
    values,
    sink,
    w_out,
    stream,
    gain,
    routes,
    route_weights,
    w_gate,
    w_up,
    w_down,
    shared_gate,
    shared_up,
    shared_down,
    *,
    nx,
):
    tok_dev = queries.shape[0]
    n_tp = lax.axis_size("tp")
    n_sp = lax.axis_size("sp")
    nz = n_sp // nx
    tp_idx = lax.axis_index("tp")
    sp_idx = lax.axis_index("sp")
    rows = tok_dev // n_tp
    d_dev = w_down.shape[2]
    exp_dev = w_gate.shape[0]
    piece = w_gate.shape[1]
    capacity = max(1, 2 * tok_dev * TOPK // (n_tp * EXPERTS))
    bf16, f32 = jnp.bfloat16, jnp.float32

    def swap(a, axis, bit):
        pairs = [(i, i ^ bit) for i in range(lax.axis_size(axis))]
        return lax.ppermute(a, axis, pairs)

    def core_swap(a):
        return swap(a, "tp", 1)

    def y_swap(a):
        return swap(a, "tp", 2)

    def x_swap(a):
        return swap(a, "sp", 1)

    def z_swap(a, bit):
        return swap(a, "sp", bit * nx)

    own_routes = lax.dynamic_slice_in_dim(routes, tp_idx * rows, rows, 0)
    own_weights = lax.dynamic_slice_in_dim(route_weights, tp_idx * rows, rows, 0)
    hits = own_routes[:, :, None] == jnp.arange(EXPERTS)[None, None, :]
    named = jnp.any(hits, axis=1)
    not_later = (jnp.arange(rows)[:, None] >= jnp.arange(rows)[None, :]).astype(bf16)
    ranks = jnp.dot(not_later, named.astype(bf16), preferred_element_type=f32)
    extra = jnp.concatenate(
        [
            jnp.where(named, ranks, 0.0),
            jnp.sum(jnp.where(hits, own_weights[:, :, None], 0.0), axis=1),
        ],
        axis=1,
    ).astype(bf16)

    attended = attention(queries, keys, values, sink)
    projected = jnp.dot(attended, w_out, preferred_element_type=f32)
    core = tp_idx % 2
    own_y = tp_idx // 2

    def quarter(y, c):
        return lax.dynamic_slice_in_dim(projected, (2 * y + c) * rows, rows, 0)

    for_away = core_swap(quarter(1 - own_y, 1 - core).astype(bf16))
    for_home = core_swap(quarter(own_y, 1 - core).astype(bf16))
    away = (quarter(1 - own_y, core) + for_away.astype(f32)).astype(bf16)
    there = y_swap(away)
    summed = quarter(own_y, core) + for_home.astype(f32) + there.astype(f32)
    mixed = (stream.astype(f32) + summed).astype(bf16)
    wide = mixed.astype(f32)
    scale = lax.rsqrt(jnp.mean(wide * wide, axis=-1, keepdims=True) + NORM_EPS)
    normed = (wide * scale * gain.astype(f32)).astype(bf16)
    own = jnp.concatenate([normed, extra], axis=1)

    chunk_z = nz // 2
    far = [own, z_swap(own, 1), z_swap(own, 2)]
    far.append(z_swap(far[2], 1))
    chunks = [([], []), ([], [])]
    for k in range(nz):
        operands, places = chunks[1 - k // chunk_z]
        by_x, by_y = x_swap(far[k]), y_swap(far[k])
        both = y_swap(by_x) if k in (1, 2) else x_swap(by_y)
        base = len(operands)
        for rows_in in (far[k], by_y, by_x, both):
            operands += [rows_in, core_swap(rows_in)]
        places += [range(base, base + n_tp), range(base + n_tp, base + 2 * n_tp)]
    quads = n_tp

    block = jnp.concatenate([part[:, :D] for part in chunks[1][0][:n_tp]], axis=0)
    shared = [
        lax.dot_general(block, w, NT, preferred_element_type=f32) for w in (shared_gate, shared_up)
    ]
    order = jnp.arange(n_tp) ^ tp_idx
    shared = silu_product(*shared).reshape(n_tp, rows, piece)
    shared = jnp.take(shared, order, axis=0).reshape(tok_dev, piece)
    shared_y = y_swap(shared)
    shared = [shared, core_swap(shared), shared_y, core_swap(shared_y)]

    def shared_of(parts):
        return sum(
            jnp.dot(
                part,
                lax.dynamic_slice_in_dim(shared_down, (tp_idx ^ place) * piece, piece, 0),
                preferred_element_type=f32,
            )
            for place, part in enumerate(parts)
        )

    def columns(a, index, width):
        return lax.dynamic_slice_in_dim(a, index * width, width, 1)

    half = 2 * d_dev
    near_y = columns(mixed, own_y, half)
    far_y = y_swap(columns(mixed, 1 - own_y, half))
    by_y = jnp.concatenate([near_y, far_y], axis=0)
    here = columns(by_y, core, d_dev)
    there = core_swap(columns(by_y, 1 - core, d_dev))

    def residual_of(here, there):
        both = jnp.stack([here[:rows], there[:rows], here[rows:], there[rows:]], axis=0)
        return jnp.take(both, order, axis=0).reshape(tok_dev, d_dev).astype(f32)

    where = jnp.stack([sp_idx * exp_dev, tp_idx]).astype(jnp.int32)
    width = quads * capacity
    lanes = exp_dev * width
    smem = pl.BlockSpec(memory_space=pltpu.SMEM)
    vmem = pl.BlockSpec(memory_space=pltpu.VMEM)
    hbm = pl.BlockSpec(memory_space=pltpu.MemorySpace.HBM)

    def in_hbm(*arrays):
        return [pltpu.with_memory_space_constraint(a, pltpu.MemorySpace.HBM) for a in arrays]

    def up_call(operands, places, own):
        units = len(places)
        shared = [shared_gate, shared_up] if own else []
        kernel = functools.partial(
            up_kernel,
            places=places,
            count=len(operands),
            own=own,
            exp_dev=exp_dev,
            capacity=capacity,
            quads=quads,
            rows=rows,
        )
        groups = exp_dev + (tok_dev // (units * width) if own else 0)
        out_shape = [
            jax.ShapeDtypeStruct((groups, units * width, piece), bf16),
            jax.ShapeDtypeStruct((units, tok_dev, lanes), bf16),
        ]
        return pl.pallas_call(
            kernel,
            in_specs=[smem] + [hbm] * (len(operands) + 2 + len(shared)),
            out_specs=[vmem] * len(out_shape),
            out_shape=out_shape,
            scratch_shapes=[
                pltpu.VMEM((RING, 2 * piece, D), bf16),
                pltpu.VMEM((exp_dev, units * width, D), bf16),
                pltpu.SemaphoreType.DMA((2, exp_dev)),
            ]
            + [pltpu.VMEM((piece, D), bf16)] * len(shared)
            + [pltpu.SemaphoreType.DMA((2,))] * (len(shared) // 2)
            + [
                pltpu.VMEM((len(operands), rows, D + LANES), bf16),
                pltpu.SemaphoreType.DMA((len(operands),)),
            ],
            compiler_params=pltpu.CompilerParams(vmem_limit_bytes=UP_VMEM),
            name="up_kernel",
        )(where, *in_hbm(*operands, w_gate, w_up, *shared))

    def down_call(hiddens, table, own):
        units = table.shape[0]
        kernel = functools.partial(
            down_kernel,
            own=own,
            units=units,
            quads=quads,
            exp_dev=exp_dev,
            capacity=capacity,
            piece=piece,
        )
        out_shape = [jax.ShapeDtypeStruct((tok_dev, d_dev), bf16)] * units
        more = []
        if own:
            out_shape = [jax.ShapeDtypeStruct((tok_dev, d_dev), f32)] + out_shape
            more = [shared_down]
        return pl.pallas_call(
            kernel,
            in_specs=[smem] + [vmem] * (quads + 1) + [hbm] * (1 + len(more)),
            out_specs=[vmem] * len(out_shape),
            out_shape=out_shape,
            scratch_shapes=[
                pltpu.VMEM((exp_dev, quads * piece, d_dev), bf16),
                pltpu.VMEM((units, lanes, d_dev), bf16),
                pltpu.SemaphoreType.DMA((exp_dev,)),
            ]
            + [pltpu.VMEM((quads * piece, d_dev), bf16), pltpu.SemaphoreType.DMA] * len(more),
            compiler_params=pltpu.CompilerParams(vmem_limit_bytes=DOWN_VMEM),
            name="down_kernel",
        )(where, *map(in_vmem, hiddens), table, *in_hbm(w_down, *more))

    sums = {}
    for chunk, (operands, places) in enumerate(chunks):
        hidden, table = up_call(operands, places, False)
        by_y = y_swap(hidden)
        hiddens = [hidden, core_swap(hidden)]
        hiddens += [by_y, core_swap(by_y)]
        parts = list(down_call(hiddens, table, False))
        if chunk == 0:
            parts, shared, ends = lax.optimization_barrier((parts, shared, (here, there)))
            total = residual_of(*ends) + shared_of(shared)
        if chunk == 1:
            from_next, parts[0] = lax.optimization_barrier((from_next, parts[0]))
        for pair in range(chunk_z):
            k = (1 - chunk) * chunk_z + pair
            there = x_swap(parts[pair * nx + 1])
            sums[k] = parts[pair * nx].astype(f32) + there.astype(f32)
        if chunk == 0:
            last, total = lax.optimization_barrier((sums[3].astype(bf16), total))
            from_next = z_swap(last, 1)
    from_far = z_swap((sums[2] + from_next.astype(f32)).astype(bf16), 2)
    total += sums[0] + z_swap(sums[1].astype(bf16), 1).astype(f32)
    return (total + from_far.astype(f32)).astype(bf16)


def solution(mesh):
    placed = (
        P("sp", "tp"),
        P("sp", None),
        P("sp", None),
        P("tp"),
        P("tp", None),
        P(("sp", "tp"), None),
        P(),
        P("sp", None),
        P("sp", None),
        P("sp", "tp", None),
        P("sp", "tp", None),
        P("sp", None, "tp"),
        P("tp", None),
        P("tp", None),
        P(None, "tp"),
    )
    n_sp, n_tp = mesh.shape["sp"], mesh.shape["tp"]
    nx = 1
    while 4 * nx * nx <= n_sp:
        nx *= 2

    pairs = nx == 2 and n_tp == 4 and n_sp == nx * 4

    def local(*args):
        tok_dev, piece = args[0].shape[0], args[9].shape[1]
        capacity = 2 * tok_dev * TOPK // (n_tp * EXPERTS)
        tiles = capacity % 8 == 0 and piece % LANES == 0 and (tok_dev // n_tp) % 16 == 0
        slots = n_sp * n_tp * capacity == tok_dev
        if pairs and tiles and slots:
            return local_torus(*args, nx=nx)
        return local_general(*args)

    return jax.shard_map(
        local, mesh=mesh, in_specs=placed, out_specs=P("sp", "tp"), check_vma=False
    )
```
